32 devices in a mesh: grp: 2 (over x), ep: 8 (over z, y), tp: 2 (over core).
Axes of the slice: x: 2, y: 2, z: 4, core: 2. Of those that a mesh axis runs over, the one named last changes fastest.
Arguments:
- tokens: bfloat16 [4096, 2048], P(('grp', 'ep', 'tp')), parts along dimension 0, may hold values from -6 to 6
- norm_gain: float32 [2048], replicated, may hold values from 0.1 to 1.9
- expert_ids: int32 [4096, 2], P(('grp', 'ep', 'tp')), parts along dimension 0, may hold values from 0 to 7, as said below
- gate_weights: float32 [4096, 2], P(('grp', 'ep', 'tp')), parts along dimension 0, may hold values from 0.1 to 1
- w_gate: bfloat16 [8, 2048, 512], P('ep', None, 'tp'), may hold values from -0.125 to 0.125
- w_up: bfloat16 [8, 2048, 512], P('ep', None, 'tp'), may hold values from -0.125 to 0.125
- w_down: bfloat16 [8, 512, 2048], P('ep', 'tp'), may hold values from -0.25 to 0.25
Outputs:
- mixed: bfloat16 [4096, 2048], P(('grp', 'ep', 'tp')), parts along dimension 0
The draws below stay inside these ranges and needn't reach their ends.
There are 2 independent parts, one for each index of `grp`. The reference program is written for one: setup_inputs(seed, part) draws one part's arguments, and reference() takes and returns one part's arrays. A program takes and returns all parts, laid end to end along the dimension named above; an argument that names none is the same for every part. Nothing has to cross between parts.
Inputs may be any that keep to these rules, and one draw needn't show every extreme that they name: `expert_ids`: the 2 experts of a token are different and lie in one group of 2 consecutive experts. Among the rows of one device (aligned blocks of 128 rows) no expert is named more than 64 times, and in every such block some expert is named exactly 64 times.
All inputs are finite; a program needn't handle non-finite values.
Results may differ from the reference program's by a relative error of at most 0.0078.
Values may be sent and summed in bfloat16 or wider, within the bound.
A program may use at most 64 MiB of HBM per device.

```python
import math
import jax
import jax.numpy as jnp
from jax import lax

D = 2048
FF = 512
N_GROUPS = 4
TOP_K = 2
TOK_DEV = 128
EXPERTS = 8
TOKENS = 2048
N_TP = 2


def draw_expert_ids(key, part):
    n_blocks = TOKENS // TOK_DEV
    per_group = EXPERTS // N_GROUPS
    half_rows = TOK_DEV // 2
    keys = jax.random.split(jax.random.fold_in(key, 17), 8)
    favored = jax.random.randint(keys[0], (), 0, N_GROUPS)
    coin = jax.random.randint(keys[1], (n_blocks,), 0, 2)
    other = jax.random.randint(keys[2], (n_blocks,), 0, N_GROUPS)
    busiest = jnp.where(coin == 1, favored, other)
    first_size = jax.random.randint(keys[3], (n_blocks,), 0, half_rows + 1)
    second_size = jax.random.randint(keys[4], (n_blocks,), 0, half_rows + 1) % (half_rows - first_size + 1)
    third_size = half_rows - first_size - second_size
    sizes = jnp.stack([jnp.full((n_blocks,), half_rows, jnp.int32), first_size, second_size, third_size], axis=1)
    ends = jnp.cumsum(sizes, axis=1)
    begins = ends - sizes
    position = jnp.arange(TOK_DEV, dtype=jnp.int32)
    rank = jnp.sum((position[None, :, None] >= ends[:, None, :]).astype(jnp.int32), axis=2)
    rank = jnp.minimum(rank, N_GROUPS - 1)
    inner = position[None, :] - jnp.take_along_axis(begins, rank, axis=1)
    group = (busiest[:, None] + rank) % N_GROUPS
    offset = jax.random.randint(keys[5], (n_blocks, 1), 0, per_group)
    stride = jax.random.randint(keys[6], (n_blocks, 1), 1, (per_group - 1) // (TOP_K - 1) + 1)
    choice_index = jnp.arange(TOP_K, dtype=jnp.int32)
    within = (offset[:, :, None] + inner[:, :, None] + choice_index[None, None, :] * stride[:, :, None]) % per_group
    by_position = group[:, :, None] * per_group + within
    orders = jax.vmap(lambda sub: jax.random.permutation(sub, TOK_DEV))(jax.random.split(keys[7], n_blocks))
    inverse = jnp.argsort(orders, axis=1, stable=True)
    by_token = jnp.take_along_axis(by_position, inverse[:, :, None], axis=1)
    return by_token.reshape(TOKENS, TOP_K).astype(jnp.int32)


def shard_levels(stream_key, dims, pieces, least, top_value):
    def one(dim, blocks):
        heights = jax.random.uniform(jax.random.fold_in(jax.random.fold_in(stream_key, 6), dim), (blocks,), jnp.float32, least / len(pieces), top_value / len(pieces))
        return jnp.repeat(jnp.exp(heights), dims[dim] // blocks).reshape((-1,) + (1,) * (len(dims) - dim - 1))

    gain = one(*pieces[0])
    for cut in pieces[1:]:
        gain = gain * one(*cut)
    return gain


def noise(own_key, shape, spread, most, cuts=(), kind=jnp.bfloat16):
    gain = shard_levels(own_key, shape, cuts, -0.22, 0.18) if cuts else 1.0
    result = jax.random.normal(own_key, shape, jnp.float32) * spread * gain
    return jnp.minimum(jnp.maximum(result, -most), most).astype(kind)


def setup_inputs(seed: int = 0, part: int = 0) -> dict:
    key_of = jax.random.split(jax.random.key(seed), 8)
    part_splits = jax.random.split(jax.random.fold_in(key_of[7], part), 8)
    return {
        "tokens": noise(part_splits[0], (TOKENS, D), 1.0, 6.0, ((0, 16),)),
        "norm_gain": jnp.clip(1.0 + 0.18 * jax.random.normal(key_of[1], (D,), jnp.float32), 0.1, 1.9),
        "expert_ids": draw_expert_ids(jax.random.fold_in(jax.random.fold_in(key_of[7], part), 71), part),
        "gate_weights": jnp.clip(jnp.exp(math.log(1.0) - 2.3025851 * jax.random.uniform(part_splits[3], (TOKENS, TOP_K), jnp.float32) ** shard_levels(part_splits[3], (TOKENS, TOP_K), ((0, 16),), -0.2, 0.2)), 0.1, 1.0),
        "w_gate": noise(key_of[4], (EXPERTS, D, FF), D ** -0.5, 0.125, ((0, 8), (2, 2))),
        "w_up": noise(key_of[5], (EXPERTS, D, FF), D ** -0.5, 0.125, ((0, 8), (2, 2))),
        "w_down": noise(key_of[6], (EXPERTS, FF, D), FF ** -0.5, 0.25, ((0, 8), (1, 2))),
    }


def reference(tokens, norm_gain, expert_ids, gate_weights, w_gate, w_up, w_down):
    values = tokens.astype(jnp.float32)
    normed = (values * lax.rsqrt(lax.optimization_barrier(jnp.mean(values * values, axis=-1, keepdims=True)) + 1e-06) * norm_gain).astype(jnp.bfloat16)
    n_tok = normed.shape[0]
    model_width = normed.shape[1]
    top_count = expert_ids.shape[1]
    total = n_tok * top_count
    block_rows = 128
    n_blocks = (total + EXPERTS * (block_rows - 1) + block_rows - 1) // block_rows
    flat_e = expert_ids.reshape(-1).astype(jnp.int32)
    flat_tok = (jnp.arange(total, dtype=jnp.int32) // top_count).astype(jnp.int32)
    sorted_order = jnp.argsort(flat_e, stable=True).astype(jnp.int32)
    sorted_e = flat_e[sorted_order]
    expert_counts = jnp.bincount(flat_e, length=EXPERTS).astype(jnp.int32)
    starts = (jnp.cumsum(expert_counts) - expert_counts).astype(jnp.int32)
    padded_counts = ((expert_counts + block_rows - 1) // block_rows * block_rows).astype(jnp.int32)
    padded_ends = jnp.cumsum(padded_counts).astype(jnp.int32)
    padded_starts = (padded_ends - padded_counts).astype(jnp.int32)
    dest_index = (padded_starts[sorted_e] + jnp.arange(total, dtype=jnp.int32) - starts[sorted_e]).astype(jnp.int32)
    rows_tok = jnp.full((n_blocks * block_rows,), n_tok, jnp.int32).at[dest_index].set(flat_tok[sorted_order])
    rows_gate = jnp.zeros((n_blocks * block_rows,), jnp.float32).at[dest_index].set(gate_weights.reshape(-1)[sorted_order])
    block_e = jnp.minimum(jnp.searchsorted(padded_ends, jnp.arange(n_blocks, dtype=jnp.int32) * block_rows, side='right'), EXPERTS - 1).astype(jnp.int32)
    x_pad = jnp.concatenate([normed, jnp.zeros((1, model_width), normed.dtype)], axis=0)
    hidden_block = FF // N_TP

    def run_block(inputs):
        expert, toks = inputs
        rows_in = x_pad[toks]
        gate_act = jnp.dot(rows_in, w_gate[expert], preferred_element_type=jnp.float32)
        up_act = jnp.dot(rows_in, w_up[expert], preferred_element_type=jnp.float32)
        hidden = (jax.nn.silu(gate_act) * up_act).astype(jnp.bfloat16)
        down = w_down[expert]
        acc = jnp.zeros((rows_in.shape[0], model_width), jnp.float32)
        for index in range(N_TP):
            partial_value = jnp.dot(hidden[:, index * hidden_block:(index + 1) * hidden_block], down[index * hidden_block:(index + 1) * hidden_block], preferred_element_type=jnp.float32)
            rounded = lax.optimization_barrier(partial_value.astype(jnp.bfloat16))
            acc = acc + rounded.astype(jnp.float32)
        return acc.astype(jnp.bfloat16)
    outputs = lax.map(run_block, (block_e, rows_tok.reshape(n_blocks, block_rows)))
    mixed = jnp.zeros((n_tok + 1, model_width), jnp.float32).at[rows_tok].add(outputs.reshape(-1, model_width).astype(jnp.float32) * rows_gate[:, None])
    return mixed[:n_tok].astype(jnp.bfloat16)
```

```python
import functools

import jax
import jax.numpy as jnp
from jax import lax
from jax.experimental import pallas as pl
from jax.experimental.pallas import tpu as pltpu
from jax.sharding import PartitionSpec as P

N_GROUPS = 4


def normalize(tokens, norm_gain):
    values = tokens.astype(jnp.float32)
    scaled = values * lax.rsqrt(jnp.mean(values * values, axis=-1, keepdims=True) + 1e-06)
    return (scaled * norm_gain).astype(jnp.bfloat16)


def expert_whole(bucket_rows, full_gate, full_up, full_down, blocks):
    gate_act = jnp.einsum(
        "secd,edf->secf", bucket_rows, full_gate, preferred_element_type=jnp.float32
    )
    up_act = jnp.einsum("secd,edf->secf", bucket_rows, full_up, preferred_element_type=jnp.float32)
    hidden = (jax.nn.silu(gate_act) * up_act).astype(jnp.bfloat16)
    width = hidden.shape[-1] // blocks
    total = jnp.zeros(bucket_rows.shape, jnp.float32)
    for index in range(blocks):
        partial_value = jnp.einsum(
            "secf,efd->secd",
            hidden[..., index * width : (index + 1) * width],
            full_down[:, index * width : (index + 1) * width, :],
            preferred_element_type=jnp.float32,
        )
        rounded = lax.optimization_barrier(partial_value.astype(jnp.bfloat16))
        total = total + rounded.astype(jnp.float32)
    return total.astype(jnp.bfloat16)


def generic_shards(tokens, norm_gain, expert_ids, gate_weights, w_gate, w_up, w_down):
    normed = normalize(tokens, norm_gain)
    n_tok, model_width = normed.shape
    top_count = expert_ids.shape[1]
    local_experts = w_gate.shape[0]
    n_ep = lax.axis_size("ep")
    n_tp = lax.axis_size("tp")
    n_exp = local_experts * n_ep
    capacity = top_count * (n_tok // 2) // (n_exp // N_GROUPS)
    total = n_tok * top_count
    n_slots = n_exp * capacity
    flat_e = expert_ids.reshape(-1)
    onehot = (flat_e[:, None] == jnp.arange(n_exp, dtype=jnp.int32)[None, :]).astype(jnp.bfloat16)
    positions = jnp.arange(total, dtype=jnp.int32)
    earlier = (positions[:, None] > positions[None, :]).astype(jnp.bfloat16)
    before = jnp.dot(earlier, onehot, preferred_element_type=jnp.float32)
    slot_index = jnp.sum(before * onehot.astype(jnp.float32), axis=1).astype(jnp.int32)
    dest_index = flat_e * capacity + slot_index
    slot_ids = jnp.arange(n_slots, dtype=jnp.int32)
    dispatch = (dest_index[None, :] == slot_ids[:, None]).astype(jnp.bfloat16)
    dispatch_tok = jnp.sum(dispatch.reshape(n_slots, n_tok, top_count), axis=2)
    buckets = jnp.dot(dispatch_tok, normed, preferred_element_type=jnp.float32).astype(jnp.bfloat16)
    buckets = buckets.reshape(n_exp, capacity, model_width)
    full_gate, full_up, full_down = (
        lax.all_gather(w_gate, "tp", axis=2, tiled=True),
        lax.all_gather(w_up, "tp", axis=2, tiled=True),
        lax.all_gather(w_down, "tp", axis=1, tiled=True),
    )
    received = lax.all_to_all(buckets, "ep", split_axis=0, concat_axis=0, tiled=True)
    grouped_rows = received.reshape(-1, local_experts, received.shape[1], model_width)
    computed = expert_whole(grouped_rows, full_gate, full_up, full_down, n_tp).reshape(
        received.shape
    )
    results = lax.all_to_all(computed, "ep", split_axis=0, concat_axis=0, tiled=True)
    results = results.reshape(n_slots, model_width)
    dest_pairs = dest_index.reshape(n_tok, top_count)
    mixed = jnp.zeros((n_tok, model_width), jnp.float32)
    for index in range(top_count):
        select = (dest_pairs[:, index][:, None] == slot_ids[None, :]).astype(jnp.bfloat16)
        picked = jnp.dot(select, results, preferred_element_type=jnp.float32)
        mixed = mixed + picked * gate_weights[:, index][:, None]
    return mixed.astype(jnp.bfloat16)


LANES = 128
MESH = pl.DeviceIdType.MESH


def route_order(n_groups, home):
    low = (home < n_groups // 2).astype(jnp.int32)
    order = [home]
    for index in range(n_groups - 1):
        up = index + (index >= home).astype(jnp.int32)
        down = n_groups - 1 - index - (index >= n_groups - 1 - home).astype(jnp.int32)
        order.append(low * up + (1 - low) * down)
    return order


def layer_kernel(
    n_groups, rows, tok_ref, gain_ref, ids_ref, gates_ref, gate_hbm, up_hbm, down_hbm, out_ref,
    sent, inbox, own, other, from_pair, back, final, gate_w, up_w, down_w, place,
    local_sem, w_send, w_recv, z_send, z_recv, y_send, y_recv, p_send, p_recv, b_send, b_recv,
):
    n_tok, width = tok_ref.shape
    half = gate_w.shape[2]
    members = 2
    ep = lax.axis_index("ep")
    core = lax.axis_index("tp")
    home = ep // members
    member = ep % members
    pair_id = {"ep": home * members + 1 - member}
    core_id = {"tp": 1 - core}
    order = route_order(n_groups, home)

    def row_id(group):
        return {"ep": group * members + member}

    locals_ = []
    for index, (src, dst) in enumerate(((gate_hbm, gate_w), (up_hbm, up_w), (down_hbm, down_w))):
        copy = pltpu.make_async_copy(src.at[0], dst.at[core], local_sem.at[index])
        copy.start()
        locals_.append(copy)

    barrier = pltpu.get_barrier_semaphore()
    for group in order[1:]:
        pl.semaphore_signal(barrier, inc=1, device_id=row_id(group), device_id_type=MESH)
    pl.semaphore_signal(barrier, inc=1, device_id=pair_id, device_id_type=MESH)
    pl.semaphore_signal(barrier, inc=1, device_id=core_id, device_id_type=MESH)

    ids = ids_ref[...]
    gates = gates_ref[...]
    group_of = ids[:, 0:1] // members
    lane = lax.broadcasted_iota(jnp.int32, (n_tok, LANES), 1)
    onehot = (group_of == lane).astype(jnp.float32)
    token = lax.broadcasted_iota(jnp.int32, (n_tok, n_tok), 0)
    earlier = (token > lax.broadcasted_iota(jnp.int32, (n_tok, n_tok), 1)).astype(jnp.bfloat16)
    before = jnp.dot(earlier, onehot.astype(jnp.bfloat16), preferred_element_type=jnp.float32)
    rank = jnp.sum(before * onehot, axis=1, keepdims=True).astype(jnp.int32)
    slot = group_of * rows + rank
    slots = lax.broadcasted_iota(jnp.int32, (n_tok, n_groups * rows), 1)
    place_t = (slot == slots).astype(jnp.float32)
    place[...] = place_t.astype(jnp.bfloat16)
    pick = place_t.T.astype(jnp.bfloat16)

    values = tok_ref[...].astype(jnp.float32)
    scale = lax.rsqrt(jnp.mean(values * values, axis=-1, keepdims=True) + 1e-06)
    normed = (values * scale * gain_ref[...]).astype(jnp.bfloat16)

    first = (ids[:, 0:1] % members) == 0
    by_member = (
        jnp.where(first, gates[:, 0:1], gates[:, 1:2]),
        jnp.where(first, gates[:, 1:2], gates[:, 0:1]),
    )
    extra = jnp.zeros((n_tok, LANES), jnp.float32)
    for index, weight in enumerate(by_member):
        left = weight
        for piece in range(3):
            part = left.astype(jnp.bfloat16).astype(jnp.float32)
            extra = jnp.where(lane == index * 3 + piece, part, extra)
            left = left - part
    extra = extra.astype(jnp.bfloat16)

    for group in range(n_groups):
        chosen = pick[group * rows : (group + 1) * rows, :]
        sent[group, :, :width] = jnp.dot(
            chosen, normed, preferred_element_type=jnp.float32
        ).astype(jnp.bfloat16)
        sent[group, :, width:] = jnp.dot(
            chosen, extra, preferred_element_type=jnp.float32
        ).astype(jnp.bfloat16)

    pl.semaphore_wait(barrier, n_groups + 1)

    def z_copy(index):
        return pltpu.make_async_remote_copy(
            src_ref=sent.at[order[index]],
            dst_ref=inbox.at[home, pl.ds(0, rows)],
            send_sem=z_send.at[index],
            recv_sem=z_recv.at[home],
            device_id=row_id(order[index]),
            device_id_type=MESH,
        )

    def z_arrival(index):
        return pltpu.make_async_remote_copy(
            src_ref=sent.at[order[index]],
            dst_ref=inbox.at[order[index], pl.ds(0, rows)],
            send_sem=z_send.at[index],
            recv_sem=z_recv.at[order[index]],
            device_id=row_id(order[index]),
            device_id_type=MESH,
        )

    def y_copy(index):
        src = sent.at[home] if index == 0 else inbox.at[order[index], pl.ds(0, rows)]
        return pltpu.make_async_remote_copy(
            src_ref=src,
            dst_ref=inbox.at[order[index], pl.ds(rows, rows)],
            send_sem=y_send.at[index],
            recv_sem=y_recv.at[index],
            device_id=pair_id,
            device_id_type=MESH,
        )

    def pair_copy(index):
        return pltpu.make_async_remote_copy(
            src_ref=other.at[index],
            dst_ref=from_pair.at[index],
            send_sem=p_send.at[index],
            recv_sem=p_recv.at[index],
            device_id=pair_id,
            device_id_type=MESH,
        )

    def back_copy(index):
        return pltpu.make_async_remote_copy(
            src_ref=back.at[index],
            dst_ref=final.at[home],
            send_sem=b_send.at[index],
            recv_sem=b_recv.at[home],
            device_id=row_id(order[index]),
            device_id_type=MESH,
        )

    def back_arrival(index):
        return pltpu.make_async_remote_copy(
            src_ref=back.at[index],
            dst_ref=final.at[order[index]],
            send_sem=b_send.at[index],
            recv_sem=b_recv.at[order[index]],
            device_id=row_id(order[index]),
            device_id_type=MESH,
        )

    for index in range(1, n_groups):
        z_copy(index).start()
    y_copy(0).start()
    shared = []
    for index, (src, dst) in enumerate(((gate_hbm, gate_w), (up_hbm, up_w), (down_hbm, down_w))):
        copy = pltpu.make_async_remote_copy(
            src_ref=src.at[0],
            dst_ref=dst.at[core],
            send_sem=w_send.at[index],
            recv_sem=w_recv.at[index],
            device_id=core_id,
            device_id_type=MESH,
        )
        copy.start()
        shared.append(copy)
    inbox[home, 0:rows, :] = sent[home]
    for copy in locals_:
        copy.wait()
    for copy in shared:
        copy.wait()

    def forward(index):
        z_arrival(index).wait_recv()
        y_copy(index).start()

    def compute(index):
        y_copy(index).wait_recv()
        group = order[index]
        x = inbox[group, :, :width]
        tail = inbox[group, :, width:].astype(jnp.float32)
        weights = [tail[:, k * 3 : k * 3 + 1] + tail[:, k * 3 + 1 : k * 3 + 2] + tail[:, k * 3 + 2 : k * 3 + 3] for k in range(2)]
        weight = jnp.where(member == 0, weights[0], weights[1])
        hidden = []
        for j in range(2):
            g = jnp.dot(x, gate_w[j], preferred_element_type=jnp.float32)
            u = jnp.dot(x, up_w[j], preferred_element_type=jnp.float32)
            hidden.append((g / (1.0 + jnp.exp(-g)) * u).astype(jnp.bfloat16))
        step = min(512, width)
        for begin in range(0, width, step):
            out = jnp.dot(
                hidden[0], down_w[0, :, begin : begin + step], preferred_element_type=jnp.float32
            ) + jnp.dot(
                hidden[1], down_w[1, :, begin : begin + step], preferred_element_type=jnp.float32
            )
            out = out * weight
            own[index, :, begin : begin + step] = out[:rows]
            other[index, :, begin : begin + step] = out[rows:].astype(jnp.bfloat16)
        pair_copy(index).start()

    def combine(index):
        pair_copy(index).wait_recv()
        total = (own[index] + from_pair[index].astype(jnp.float32)).astype(jnp.bfloat16)
        if index == 0:
            final[home] = total
        else:
            back[index] = total
            back_copy(index).start()

    forward(1)
    compute(0)
    for index in range(2, n_groups):
        forward(index)
        compute(index - 1)
        combine(index - 2)
    compute(n_groups - 1)
    combine(n_groups - 2)
    combine(n_groups - 1)
    for index in range(1, n_groups):
        back_arrival(index).wait_recv()
    mixed = jnp.dot(
        place[...], final[...].reshape(n_groups * rows, width), preferred_element_type=jnp.float32
    )
    out_ref[...] = mixed.astype(out_ref.dtype)
    for index in range(n_groups):
        if index:
            z_copy(index).wait_send()
            back_copy(index).wait_send()
        y_copy(index).wait_send()
        pair_copy(index).wait_send()


def shards(tokens, norm_gain, expert_ids, gate_weights, w_gate, w_up, w_down):
    n_tok, width = tokens.shape
    local_experts = w_gate.shape[0]
    n_exp = local_experts * lax.axis_size("ep")
    per_group = n_exp // N_GROUPS
    top_count = expert_ids.shape[1]
    if not (local_experts == 1 and per_group == 2 and top_count == 2 and lax.axis_size("tp") == 2):
        return generic_shards(tokens, norm_gain, expert_ids, gate_weights, w_gate, w_up, w_down)
    rows = n_tok // 2
    half = w_gate.shape[2]
    bf16, f32 = jnp.bfloat16, jnp.float32
    dma = pltpu.SemaphoreType.DMA
    vmem = pl.BlockSpec(memory_space=pltpu.VMEM)
    hbm = pl.BlockSpec(memory_space=pl.ANY)
    return pl.pallas_call(
        functools.partial(layer_kernel, N_GROUPS, rows),
        out_shape=jax.ShapeDtypeStruct((n_tok, width), bf16),
        in_specs=[vmem] * 4 + [hbm] * 3,
        out_specs=vmem,
        scratch_shapes=[
            pltpu.VMEM((N_GROUPS, rows, width + LANES), bf16),
            pltpu.VMEM((N_GROUPS, 2 * rows, width + LANES), bf16),
            pltpu.VMEM((N_GROUPS, rows, width), f32),
            pltpu.VMEM((N_GROUPS, rows, width), bf16),
            pltpu.VMEM((N_GROUPS, rows, width), bf16),
            pltpu.VMEM((N_GROUPS, rows, width), bf16),
            pltpu.VMEM((N_GROUPS, rows, width), bf16),
            pltpu.VMEM((2, width, half), bf16),
            pltpu.VMEM((2, width, half), bf16),
            pltpu.VMEM((2, half, width), bf16),
            pltpu.VMEM((n_tok, N_GROUPS * rows), bf16),
            dma((3,)), dma((3,)), dma((3,)),
        ] + [dma((N_GROUPS,))] * 8,
        compiler_params=pltpu.CompilerParams(
            collective_id=0, has_side_effects=True, vmem_limit_bytes=48 * 1024 * 1024
        ),
        name="expert_layer",
    )(tokens, norm_gain.reshape(1, width), expert_ids, gate_weights, w_gate, w_up, w_down)


def solution(mesh):
    placed = (
        P(("grp", "ep", "tp"), None),
        P(),
        P(("grp", "ep", "tp"), None),
        P(("grp", "ep", "tp"), None),
        P("ep", None, "tp"),
        P("ep", None, "tp"),
        P("ep", "tp", None),
    )
    return jax.shard_map(
        shards, mesh=mesh, in_specs=placed, out_specs=P(("grp", "ep", "tp"), None), check_vma=False
    )
```

```python
import functools

import jax
import jax.numpy as jnp
from jax import lax
from jax.experimental import pallas as pl
from jax.experimental.pallas import tpu as pltpu
from jax.sharding import PartitionSpec as P

N_GROUPS = 4


def normalize(tokens, norm_gain):
    values = tokens.astype(jnp.float32)
    scaled = values * lax.rsqrt(jnp.mean(values * values, axis=-1, keepdims=True) + 1e-06)
    return (scaled * norm_gain).astype(jnp.bfloat16)


def expert_whole(bucket_rows, full_gate, full_up, full_down, blocks):
    gate_act = jnp.einsum(
        "secd,edf->secf", bucket_rows, full_gate, preferred_element_type=jnp.float32
    )
    up_act = jnp.einsum("secd,edf->secf", bucket_rows, full_up, preferred_element_type=jnp.float32)
    hidden = (jax.nn.silu(gate_act) * up_act).astype(jnp.bfloat16)
    width = hidden.shape[-1] // blocks
    total = jnp.zeros(bucket_rows.shape, jnp.float32)
    for index in range(blocks):
        partial_value = jnp.einsum(
            "secf,efd->secd",
            hidden[..., index * width : (index + 1) * width],
            full_down[:, index * width : (index + 1) * width, :],
            preferred_element_type=jnp.float32,
        )
        rounded = lax.optimization_barrier(partial_value.astype(jnp.bfloat16))
        total = total + rounded.astype(jnp.float32)
    return total.astype(jnp.bfloat16)


def generic_shards(tokens, norm_gain, expert_ids, gate_weights, w_gate, w_up, w_down):
    normed = normalize(tokens, norm_gain)
    n_tok, model_width = normed.shape
    top_count = expert_ids.shape[1]
    local_experts = w_gate.shape[0]
    n_ep = lax.axis_size("ep")
    n_tp = lax.axis_size("tp")
    n_exp = local_experts * n_ep
    capacity = top_count * (n_tok // 2) // (n_exp // N_GROUPS)
    total = n_tok * top_count
    n_slots = n_exp * capacity
    flat_e = expert_ids.reshape(-1)
    onehot = (flat_e[:, None] == jnp.arange(n_exp, dtype=jnp.int32)[None, :]).astype(jnp.bfloat16)
    positions = jnp.arange(total, dtype=jnp.int32)
    earlier = (positions[:, None] > positions[None, :]).astype(jnp.bfloat16)
    before = jnp.dot(earlier, onehot, preferred_element_type=jnp.float32)
    slot_index = jnp.sum(before * onehot.astype(jnp.float32), axis=1).astype(jnp.int32)
    dest_index = flat_e * capacity + slot_index
    slot_ids = jnp.arange(n_slots, dtype=jnp.int32)
    dispatch = (dest_index[None, :] == slot_ids[:, None]).astype(jnp.bfloat16)
    dispatch_tok = jnp.sum(dispatch.reshape(n_slots, n_tok, top_count), axis=2)
    buckets = jnp.dot(dispatch_tok, normed, preferred_element_type=jnp.float32).astype(jnp.bfloat16)
    buckets = buckets.reshape(n_exp, capacity, model_width)
    full_gate, full_up, full_down = (
        lax.all_gather(w_gate, "tp", axis=2, tiled=True),
        lax.all_gather(w_up, "tp", axis=2, tiled=True),
        lax.all_gather(w_down, "tp", axis=1, tiled=True),
    )
    received = lax.all_to_all(buckets, "ep", split_axis=0, concat_axis=0, tiled=True)
    grouped_rows = received.reshape(-1, local_experts, received.shape[1], model_width)
    computed = expert_whole(grouped_rows, full_gate, full_up, full_down, n_tp).reshape(
        received.shape
    )
    results = lax.all_to_all(computed, "ep", split_axis=0, concat_axis=0, tiled=True)
    results = results.reshape(n_slots, model_width)
    dest_pairs = dest_index.reshape(n_tok, top_count)
    mixed = jnp.zeros((n_tok, model_width), jnp.float32)
    for index in range(top_count):
        select = (dest_pairs[:, index][:, None] == slot_ids[None, :]).astype(jnp.bfloat16)
        picked = jnp.dot(select, results, preferred_element_type=jnp.float32)
        mixed = mixed + picked * gate_weights[:, index][:, None]
    return mixed.astype(jnp.bfloat16)


LANES = 128
MESH = pl.DeviceIdType.MESH


def route_order(n_groups, home):
    low = (home < n_groups // 2).astype(jnp.int32)
    rim = low * home + (1 - low) * (n_groups - 1 - home)
    order = [home]
    for index in range(n_groups - 1):
        inner = (index < 2 * rim).astype(jnp.int32)
        step = index // 2 + 1 if index % 2 == 0 else -(index // 2 + 1)
        at = inner * (rim + step) + (1 - inner) * (index + 1)
        order.append(low * at + (1 - low) * (n_groups - 1 - at))
    return order


def layer_kernel(
    n_groups, rows, tok_hbm, gain_ref, ids_ref, gates_ref, gate_hbm, up_hbm, down_hbm, out_ref,
    tok, pick_ref, sent, inbox, own, other, from_pair, back, final, gate_w, up_w, down_w, place,
    local_sem, w_send, w_recv, z_send, z_recv, y_send, y_recv, p_send, p_recv, b_send, b_recv,
):
    n_tok, width = tok.shape
    members = 2
    pieces = 2
    cut = rows // pieces
    ep = lax.axis_index("ep")
    core = lax.axis_index("tp")
    home = ep // members
    member = ep % members
    pair_id = {"ep": home * members + 1 - member}
    core_id = {"tp": 1 - core}
    order = route_order(n_groups, home)
    at_end = jnp.logical_or(home == 0, home == n_groups - 1)

    def row_id(group):
        return {"ep": group * members + member}

    def remote(src, dst, send, recv, target):
        return pltpu.make_async_remote_copy(
            src_ref=src, dst_ref=dst, send_sem=send, recv_sem=recv,
            device_id=target, device_id_type=MESH,
        )

    tok_copy = pltpu.make_async_copy(tok_hbm, tok, local_sem.at[3])
    tok_copy.start()
    barrier = pltpu.get_barrier_semaphore()
    for group in order[1:]:
        pl.semaphore_signal(barrier, inc=1, device_id=row_id(group), device_id_type=MESH)
    pl.semaphore_signal(barrier, inc=1, device_id=pair_id, device_id_type=MESH)
    pl.semaphore_signal(barrier, inc=1, device_id=core_id, device_id_type=MESH)
    weights = ((gate_hbm, gate_w), (up_hbm, up_w), (down_hbm, down_w))
    loads = [
        pltpu.make_async_copy(src.at[0], dst.at[core], local_sem.at[index])
        for index, (src, dst) in enumerate(weights)
    ]
    for copy in loads:
        copy.start()

    token = lax.broadcasted_iota(jnp.int32, (n_tok, n_tok), 0)
    lane = lax.broadcasted_iota(jnp.int32, (n_tok, n_tok), 1)
    eye = token == lane

    def column(row):
        return jnp.sum(jnp.where(eye, row, jnp.zeros_like(row)), axis=1, keepdims=True)

    first_id = ids_ref[0:1, :]
    group_row = first_id // members
    group_of = column(group_row)
    onehot = (group_of == lane).astype(jnp.float32)
    earlier = (token > lane).astype(jnp.bfloat16)
    before = jnp.dot(earlier, onehot.astype(jnp.bfloat16), preferred_element_type=jnp.float32)
    rank = jnp.sum(before * onehot, axis=1, keepdims=True).astype(jnp.int32)
    slot = group_of * rows + rank
    slots = lax.broadcasted_iota(jnp.int32, (n_tok, n_groups * rows), 1)
    place_t = (slot == slots).astype(jnp.float32)
    place[...] = place_t.astype(jnp.bfloat16)
    pick_ref[...] = place_t.T.astype(jnp.bfloat16).reshape(pick_ref.shape)

    first = (first_id % members) == 0
    by_member = (
        jnp.where(first, gates_ref[0:1, :], gates_ref[1:2, :]),
        jnp.where(first, gates_ref[1:2, :], gates_ref[0:1, :]),
    )
    extra_lane = lax.broadcasted_iota(jnp.int32, (n_tok, LANES), 1)
    extra = jnp.zeros((n_tok, LANES), jnp.float32)
    for index, weight in enumerate(by_member):
        left = column(weight)
        for piece in range(3):
            part = left.astype(jnp.bfloat16).astype(jnp.float32)
            extra = jnp.where(extra_lane == index * 3 + piece, part, extra)
            left = left - part
    extra = extra.astype(jnp.bfloat16)

    tok_copy.wait()
    values = tok[...].astype(jnp.float32)
    scale = lax.rsqrt(jnp.mean(values * values, axis=-1, keepdims=True) + 1e-06)
    normed = (values * scale * gain_ref[...]).astype(jnp.bfloat16)

    def bucket(index):
        chosen = pick_ref[order[index]]
        main = jnp.dot(chosen, normed, preferred_element_type=jnp.float32).astype(jnp.bfloat16)
        side = jnp.dot(chosen, extra, preferred_element_type=jnp.float32).astype(jnp.bfloat16)
        if index == 0:
            inbox[home, 0:rows, :width] = main
            inbox[home, 0:rows, width:] = side
        else:
            sent[index - 1, :, :width] = main
            sent[index - 1, :, width:] = side

    def z_copy(index, piece, source=None):
        source = home if source is None else source
        return remote(
            sent.at[index - 1, pl.ds(piece * cut, cut)],
            inbox.at[source, pl.ds(piece * cut, cut)],
            z_send.at[index, piece],
            z_recv.at[source, piece],
            row_id(order[index]),
        )

    def y_copy(index, piece):
        return remote(
            inbox.at[order[index], pl.ds(piece * cut, cut)],
            inbox.at[order[index], pl.ds(rows + piece * cut, cut)],
            y_send.at[index, piece],
            y_recv.at[index, piece],
            pair_id,
        )

    def pair_copy(index, piece):
        return remote(
            other.at[index, pl.ds(piece * cut, cut)],
            from_pair.at[index, pl.ds(piece * cut, cut)],
            p_send.at[index, piece],
            p_recv.at[index, piece],
            pair_id,
        )

    def back_copy(index, piece, source=None):
        source = home if source is None else source
        return remote(
            back.at[index, pl.ds(piece * cut, cut)],
            final.at[source, pl.ds(piece * cut, cut)],
            b_send.at[index, piece],
            b_recv.at[source, piece],
            row_id(order[index]),
        )

    pl.semaphore_wait(barrier, n_groups + 1)
    shared = [
        remote(src.at[0], dst.at[core], w_send.at[index], w_recv.at[index], core_id)
        for index, (src, dst) in enumerate(weights)
    ]
    for copy in shared:
        copy.start()
    for index in (1, 0) + tuple(range(2, n_groups)):
        bucket(index)
        for piece in range(pieces):
            (z_copy(index, piece) if index else y_copy(0, piece)).start()
    for copy in loads:
        copy.wait()
    for copy in shared:
        copy.wait()

    def forward(index):
        for piece in range(pieces):
            z_copy(index, piece, order[index]).wait_recv()
            y_copy(index, piece).start()

    def compute(index):
        for piece in range(pieces):
            y_copy(index, piece).wait_recv()
        group = order[index]
        x = inbox[group, :, :width]
        tail = inbox[group, :, width:].astype(jnp.float32)
        by_expert = [
            tail[:, k : k + 1] + tail[:, k + 1 : k + 2] + tail[:, k + 2 : k + 3] for k in (0, 3)
        ]
        weight = jnp.where(member == 0, by_expert[0], by_expert[1])
        hidden = []
        for j in range(2):
            g = jnp.dot(x, gate_w[j], preferred_element_type=jnp.float32)
            u = jnp.dot(x, up_w[j], preferred_element_type=jnp.float32)
            hidden.append((g / (1.0 + jnp.exp(-g)) * u).astype(jnp.bfloat16))
        step = min(512, width)
        for begin in range(0, width, step):
            out = jnp.dot(
                hidden[0], down_w[0, :, begin : begin + step], preferred_element_type=jnp.float32
            ) + jnp.dot(
                hidden[1], down_w[1, :, begin : begin + step], preferred_element_type=jnp.float32
            )
            out = out * weight
            own[index, :, begin : begin + step] = out[:rows]
            other[index, :, begin : begin + step] = out[rows:].astype(jnp.bfloat16)

    def give(index):
        for piece in range(pieces):
            pair_copy(index, piece).start()

    def combine(index):
        for piece in range(pieces):
            pair_copy(index, piece).wait_recv()
            at = slice(piece * cut, (piece + 1) * cut)
            total = own[index, at] + from_pair[index, at].astype(jnp.float32)
            total = total.astype(jnp.bfloat16)
            if index == 0:
                final[home, at] = total
            else:
                back[index, at] = total
                back_copy(index, piece).start()

    last = n_groups - 1
    forward(1)
    if last > 2:
        pl.when(jnp.logical_not(at_end))(lambda: forward(2))
    compute(0)
    compute(1)
    give(1)
    if last > 2:
        pl.when(at_end)(lambda: forward(2))
    for index in range(3 if last > 2 else 2, n_groups):
        forward(index)
    combine(1)
    for index in range(2, n_groups):
        compute(index)
        give(index)
    give(0)
    for index in range(2, n_groups):
        combine(index)
    combine(0)
    for index in range(1, n_groups):
        for piece in range(pieces):
            back_copy(index, piece, order[index]).wait_recv()
    mixed = jnp.dot(
        place[...], final[...].reshape(n_groups * rows, width), preferred_element_type=jnp.float32
    )
    out_ref[...] = mixed.astype(out_ref.dtype)
    for index in range(n_groups):
        for piece in range(pieces):
            if index:
                z_copy(index, piece).wait_send()
                back_copy(index, piece).wait_send()
            y_copy(index, piece).wait_send()
            pair_copy(index, piece).wait_send()


def shards(tokens, norm_gain, expert_ids, gate_weights, w_gate, w_up, w_down):
    n_tok, width = tokens.shape
    local_experts = w_gate.shape[0]
    n_exp = local_experts * lax.axis_size("ep")
    per_group = n_exp // N_GROUPS
    top_count = expert_ids.shape[1]
    if not (local_experts == 1 and per_group == 2 and top_count == 2 and lax.axis_size("tp") == 2):
        return generic_shards(tokens, norm_gain, expert_ids, gate_weights, w_gate, w_up, w_down)
    rows = n_tok // 2
    half = w_gate.shape[2]
    bf16, f32 = jnp.bfloat16, jnp.float32
    dma = pltpu.SemaphoreType.DMA
    vmem = pl.BlockSpec(memory_space=pltpu.VMEM)
    hbm = pl.BlockSpec(memory_space=pl.ANY)
    return pl.pallas_call(
        functools.partial(layer_kernel, N_GROUPS, rows),
        out_shape=jax.ShapeDtypeStruct((n_tok, width), bf16),
        in_specs=[hbm] + [vmem] * 3 + [hbm] * 3,
        out_specs=vmem,
        scratch_shapes=[
            pltpu.VMEM((n_tok, width), bf16),
            pltpu.VMEM((N_GROUPS, rows, n_tok), bf16),
            pltpu.VMEM((N_GROUPS - 1, rows, width + LANES), bf16),
            pltpu.VMEM((N_GROUPS, 2 * rows, width + LANES), bf16),
            pltpu.VMEM((N_GROUPS, rows, width), f32),
            pltpu.VMEM((N_GROUPS, rows, width), bf16),
            pltpu.VMEM((N_GROUPS, rows, width), bf16),
            pltpu.VMEM((N_GROUPS, rows, width), bf16),
            pltpu.VMEM((N_GROUPS, rows, width), bf16),
            pltpu.VMEM((2, width, half), bf16),
            pltpu.VMEM((2, width, half), bf16),
            pltpu.VMEM((2, half, width), bf16),
            pltpu.VMEM((n_tok, N_GROUPS * rows), bf16),
            dma((4,)), dma((3,)), dma((3,)),
        ] + [dma((N_GROUPS, 2))] * 8,
        compiler_params=pltpu.CompilerParams(
            collective_id=0, has_side_effects=True, vmem_limit_bytes=67043328
        ),
        name="expert_layer",
    )(tokens, norm_gain.reshape(1, width), expert_ids.T, gate_weights.T, w_gate, w_up, w_down)


def solution(mesh):
    placed = (
        P(("grp", "ep", "tp"), None),
        P(),
        P(("grp", "ep", "tp"), None),
        P(("grp", "ep", "tp"), None),
        P("ep", None, "tp"),
        P("ep", None, "tp"),
        P("ep", "tp", None),
    )
    return jax.shard_map(
        shards, mesh=mesh, in_specs=placed, out_specs=P(("grp", "ep", "tp"), None), check_vma=False
    )
```

```python
import functools

import jax
import jax.numpy as jnp
from jax import lax
from jax.experimental import pallas as pl
from jax.experimental.pallas import tpu as pltpu
from jax.sharding import PartitionSpec as P

N_GROUPS = 4


def normalize(tokens, norm_gain):
    values = tokens.astype(jnp.float32)
    scaled = values * lax.rsqrt(jnp.mean(values * values, axis=-1, keepdims=True) + 1e-06)
    return (scaled * norm_gain).astype(jnp.bfloat16)


def expert_whole(bucket_rows, full_gate, full_up, full_down, blocks):
    gate_act = jnp.einsum(
        "secd,edf->secf", bucket_rows, full_gate, preferred_element_type=jnp.float32
    )
    up_act = jnp.einsum("secd,edf->secf", bucket_rows, full_up, preferred_element_type=jnp.float32)
    hidden = (jax.nn.silu(gate_act) * up_act).astype(jnp.bfloat16)
    width = hidden.shape[-1] // blocks
    total = jnp.zeros(bucket_rows.shape, jnp.float32)
    for index in range(blocks):
        partial_value = jnp.einsum(
            "secf,efd->secd",
            hidden[..., index * width : (index + 1) * width],
            full_down[:, index * width : (index + 1) * width, :],
            preferred_element_type=jnp.float32,
        )
        rounded = lax.optimization_barrier(partial_value.astype(jnp.bfloat16))
        total = total + rounded.astype(jnp.float32)
    return total.astype(jnp.bfloat16)


def generic_shards(tokens, norm_gain, expert_ids, gate_weights, w_gate, w_up, w_down):
    normed = normalize(tokens, norm_gain)
    n_tok, model_width = normed.shape
    top_count = expert_ids.shape[1]
    local_experts = w_gate.shape[0]
    n_ep = lax.axis_size("ep")
    n_tp = lax.axis_size("tp")
    n_exp = local_experts * n_ep
    capacity = top_count * (n_tok // 2) // (n_exp // N_GROUPS)
    total = n_tok * top_count
    n_slots = n_exp * capacity
    flat_e = expert_ids.reshape(-1)
    onehot = (flat_e[:, None] == jnp.arange(n_exp, dtype=jnp.int32)[None, :]).astype(jnp.bfloat16)
    positions = jnp.arange(total, dtype=jnp.int32)
    earlier = (positions[:, None] > positions[None, :]).astype(jnp.bfloat16)
    before = jnp.dot(earlier, onehot, preferred_element_type=jnp.float32)
    slot_index = jnp.sum(before * onehot.astype(jnp.float32), axis=1).astype(jnp.int32)
    dest_index = flat_e * capacity + slot_index
    slot_ids = jnp.arange(n_slots, dtype=jnp.int32)
    dispatch = (dest_index[None, :] == slot_ids[:, None]).astype(jnp.bfloat16)
    dispatch_tok = jnp.sum(dispatch.reshape(n_slots, n_tok, top_count), axis=2)
    buckets = jnp.dot(dispatch_tok, normed, preferred_element_type=jnp.float32).astype(jnp.bfloat16)
    buckets = buckets.reshape(n_exp, capacity, model_width)
    full_gate, full_up, full_down = (
        lax.all_gather(w_gate, "tp", axis=2, tiled=True),
        lax.all_gather(w_up, "tp", axis=2, tiled=True),
        lax.all_gather(w_down, "tp", axis=1, tiled=True),
    )
    received = lax.all_to_all(buckets, "ep", split_axis=0, concat_axis=0, tiled=True)
    grouped_rows = received.reshape(-1, local_experts, received.shape[1], model_width)
    computed = expert_whole(grouped_rows, full_gate, full_up, full_down, n_tp).reshape(
        received.shape
    )
    results = lax.all_to_all(computed, "ep", split_axis=0, concat_axis=0, tiled=True)
    results = results.reshape(n_slots, model_width)
    dest_pairs = dest_index.reshape(n_tok, top_count)
    mixed = jnp.zeros((n_tok, model_width), jnp.float32)
    for index in range(top_count):
        select = (dest_pairs[:, index][:, None] == slot_ids[None, :]).astype(jnp.bfloat16)
        picked = jnp.dot(select, results, preferred_element_type=jnp.float32)
        mixed = mixed + picked * gate_weights[:, index][:, None]
    return mixed.astype(jnp.bfloat16)


LANES = 128
MESH = pl.DeviceIdType.MESH


def route_order(n_groups, home):
    low = (home < n_groups // 2).astype(jnp.int32)
    rim = low * home + (1 - low) * (n_groups - 1 - home)
    order = [home]
    for index in range(n_groups - 1):
        inner = (index < 2 * rim).astype(jnp.int32)
        step = index // 2 + 1 if index % 2 == 0 else -(index // 2 + 1)
        at = inner * (rim + step) + (1 - inner) * (index + 1)
        order.append(low * at + (1 - low) * (n_groups - 1 - at))
    return order


def layer_kernel(
    n_groups, rows, tok_hbm, gain_ref, ids_ref, gates_ref, gate_hbm, up_hbm, down_hbm, out_ref,
    tok, pick_ref, sent, inbox, own, other, from_pair, back, final, gate_w, up_w, down_w, place,
    local_sem, w_send, w_recv, z_send, z_recv, y_send, y_recv, p_send, p_recv, b_send, b_recv,
):
    n_tok, width = tok.shape
    members = 2
    pieces = 4
    cut = rows // pieces
    ep = lax.axis_index("ep")
    core = lax.axis_index("tp")
    home = ep // members
    member = ep % members
    pair_id = {"ep": home * members + 1 - member}
    core_id = {"tp": 1 - core}
    order = route_order(n_groups, home)
    at_end = jnp.logical_or(home == 0, home == n_groups - 1)

    def row_id(group):
        return {"ep": group * members + member}

    def remote(src, dst, send, recv, target):
        return pltpu.make_async_remote_copy(
            src_ref=src, dst_ref=dst, send_sem=send, recv_sem=recv,
            device_id=target, device_id_type=MESH,
        )

    tok_copy = pltpu.make_async_copy(tok_hbm, tok, local_sem.at[3])
    tok_copy.start()
    barrier = pltpu.get_barrier_semaphore()
    for group in order[1:]:
        pl.semaphore_signal(barrier, inc=1, device_id=row_id(group), device_id_type=MESH)
    pl.semaphore_signal(barrier, inc=1, device_id=pair_id, device_id_type=MESH)
    pl.semaphore_signal(barrier, inc=1, device_id=core_id, device_id_type=MESH)
    weights = ((gate_hbm, gate_w), (up_hbm, up_w), (down_hbm, down_w))
    loads = [
        pltpu.make_async_copy(src.at[0], dst.at[core], local_sem.at[index])
        for index, (src, dst) in enumerate(weights)
    ]
    for copy in loads:
        copy.start()

    token = lax.broadcasted_iota(jnp.int32, (n_tok, n_tok), 0)
    lane = lax.broadcasted_iota(jnp.int32, (n_tok, n_tok), 1)
    eye = token == lane

    def column(row):
        return jnp.sum(jnp.where(eye, row, jnp.zeros_like(row)), axis=1, keepdims=True)

    first_id = ids_ref[0:1, :]
    group_row = first_id // members
    group_of = column(group_row)
    onehot = (group_of == lane).astype(jnp.float32)
    earlier = (token > lane).astype(jnp.bfloat16)
    before = jnp.dot(earlier, onehot.astype(jnp.bfloat16), preferred_element_type=jnp.float32)
    rank = jnp.sum(before * onehot, axis=1, keepdims=True).astype(jnp.int32)
    slot = group_of * rows + rank
    slots = lax.broadcasted_iota(jnp.int32, (n_tok, n_groups * rows), 1)
    place_t = (slot == slots).astype(jnp.float32)
    place[...] = place_t.astype(jnp.bfloat16)
    pick_ref[...] = place_t.T.astype(jnp.bfloat16).reshape(pick_ref.shape)

    first = (first_id % members) == 0
    by_member = (
        jnp.where(first, gates_ref[0:1, :], gates_ref[1:2, :]),
        jnp.where(first, gates_ref[1:2, :], gates_ref[0:1, :]),
    )
    extra_lane = lax.broadcasted_iota(jnp.int32, (n_tok, LANES), 1)
    extra = jnp.zeros((n_tok, LANES), jnp.float32)
    for index, weight in enumerate(by_member):
        left = column(weight)
        for piece in range(3):
            part = left.astype(jnp.bfloat16).astype(jnp.float32)
            extra = jnp.where(extra_lane == index * 3 + piece, part, extra)
            left = left - part
    extra = extra.astype(jnp.bfloat16)

    tok_copy.wait()
    values = tok[...].astype(jnp.float32)
    scale = lax.rsqrt(jnp.mean(values * values, axis=-1, keepdims=True) + 1e-06)
    normed = (values * scale * gain_ref[...]).astype(jnp.bfloat16)

    def bucket(index):
        chosen = pick_ref[order[index]]
        main = jnp.dot(chosen, normed, preferred_element_type=jnp.float32).astype(jnp.bfloat16)
        side = jnp.dot(chosen, extra, preferred_element_type=jnp.float32).astype(jnp.bfloat16)
        if index == 0:
            inbox[home, 0:rows, :width] = main
            inbox[home, 0:rows, width:] = side
        else:
            sent[index - 1, :, :width] = main
            sent[index - 1, :, width:] = side

    def z_copy(index, piece, source=None):
        source = home if source is None else source
        return remote(
            sent.at[index - 1, pl.ds(piece * cut, cut)],
            inbox.at[source, pl.ds(piece * cut, cut)],
            z_send.at[index, piece],
            z_recv.at[source, piece],
            row_id(order[index]),
        )

    def y_copy(index, piece):
        return remote(
            inbox.at[order[index], pl.ds(piece * cut, cut)],
            inbox.at[order[index], pl.ds(rows + piece * cut, cut)],
            y_send.at[index, piece],
            y_recv.at[index, piece],
            pair_id,
        )

    def pair_copy(index, piece):
        return remote(
            other.at[index, pl.ds(piece * cut, cut)],
            from_pair.at[index, pl.ds(piece * cut, cut)],
            p_send.at[index, piece],
            p_recv.at[index, piece],
            pair_id,
        )

    def back_copy(index, piece, source=None):
        source = home if source is None else source
        return remote(
            back.at[index, pl.ds(piece * cut, cut)],
            final.at[source, pl.ds(piece * cut, cut)],
            b_send.at[index, piece],
            b_recv.at[source, piece],
            row_id(order[index]),
        )

    pl.semaphore_wait(barrier, n_groups + 1)
    shared = [
        remote(src.at[0], dst.at[core], w_send.at[index], w_recv.at[index], core_id)
        for index, (src, dst) in enumerate(weights)
    ]
    for copy in shared:
        copy.start()
    for index in (1, 0) + tuple(range(2, n_groups)):
        bucket(index)
        for piece in range(pieces):
            (z_copy(index, piece) if index else y_copy(0, piece)).start()
    for copy in loads:
        copy.wait()
    for copy in shared:
        copy.wait()

    def forward(index):
        for piece in range(pieces):
            z_copy(index, piece, order[index]).wait_recv()
            y_copy(index, piece).start()

    def compute(index):
        for piece in range(pieces):
            y_copy(index, piece).wait_recv()
        group = order[index]
        x = inbox[group, :, :width]
        tail = inbox[group, :, width:].astype(jnp.float32)
        by_expert = [
            tail[:, k : k + 1] + tail[:, k + 1 : k + 2] + tail[:, k + 2 : k + 3] for k in (0, 3)
        ]
        weight = jnp.where(member == 0, by_expert[0], by_expert[1])
        hidden = []
        for j in range(2):
            g = jnp.dot(x, gate_w[j], preferred_element_type=jnp.float32)
            u = jnp.dot(x, up_w[j], preferred_element_type=jnp.float32)
            hidden.append((g / (1.0 + jnp.exp(-g)) * u).astype(jnp.bfloat16))
        step = min(512, width)
        for begin in range(0, width, step):
            out = jnp.dot(
                hidden[0], down_w[0, :, begin : begin + step], preferred_element_type=jnp.float32
            ) + jnp.dot(
                hidden[1], down_w[1, :, begin : begin + step], preferred_element_type=jnp.float32
            )
            out = out * weight
            own[index, :, begin : begin + step] = out[:rows]
            other[index, :, begin : begin + step] = out[rows:].astype(jnp.bfloat16)

    def give(index):
        for piece in range(pieces):
            pair_copy(index, piece).start()

    def combine(index):
        for piece in range(pieces):
            pair_copy(index, piece).wait_recv()
            at = slice(piece * cut, (piece + 1) * cut)
            total = own[index, at] + from_pair[index, at].astype(jnp.float32)
            total = total.astype(jnp.bfloat16)
            if index == 0:
                final[home, at] = total
            else:
                back[index, at] = total
                back_copy(index, piece).start()

    last = n_groups - 1
    forward(1)
    if last > 2:
        pl.when(jnp.logical_not(at_end))(lambda: forward(2))
    compute(0)
    compute(1)
    give(1)
    if last > 2:
        pl.when(at_end)(lambda: forward(2))
    for index in range(3 if last > 2 else 2, n_groups):
        forward(index)
    combine(1)
    for index in range(2, n_groups):
        compute(index)
        give(index)
    give(0)
    for index in range(2, n_groups):
        combine(index)
    combine(0)
    for index in range(1, n_groups):
        for piece in range(pieces):
            back_copy(index, piece, order[index]).wait_recv()
    mixed = jnp.dot(
        place[...], final[...].reshape(n_groups * rows, width), preferred_element_type=jnp.float32
    )
    out_ref[...] = mixed.astype(out_ref.dtype)
    for index in range(n_groups):
        for piece in range(pieces):
            if index:
                z_copy(index, piece).wait_send()
                back_copy(index, piece).wait_send()
            y_copy(index, piece).wait_send()
            pair_copy(index, piece).wait_send()


def shards(tokens, norm_gain, expert_ids, gate_weights, w_gate, w_up, w_down):
    n_tok, width = tokens.shape
    local_experts = w_gate.shape[0]
    n_exp = local_experts * lax.axis_size("ep")
    per_group = n_exp // N_GROUPS
    top_count = expert_ids.shape[1]
    if not (local_experts == 1 and per_group == 2 and top_count == 2 and lax.axis_size("tp") == 2):
        return generic_shards(tokens, norm_gain, expert_ids, gate_weights, w_gate, w_up, w_down)
    rows = n_tok // 2
    half = w_gate.shape[2]
    bf16, f32 = jnp.bfloat16, jnp.float32
    dma = pltpu.SemaphoreType.DMA
    vmem = pl.BlockSpec(memory_space=pltpu.VMEM)
    hbm = pl.BlockSpec(memory_space=pl.ANY)
    return pl.pallas_call(
        functools.partial(layer_kernel, N_GROUPS, rows),
        out_shape=jax.ShapeDtypeStruct((n_tok, width), bf16),
        in_specs=[hbm] + [vmem] * 3 + [hbm] * 3,
        out_specs=vmem,
        scratch_shapes=[
            pltpu.VMEM((n_tok, width), bf16),
            pltpu.VMEM((N_GROUPS, rows, n_tok), bf16),
            pltpu.VMEM((N_GROUPS - 1, rows, width + LANES), bf16),
            pltpu.VMEM((N_GROUPS, 2 * rows, width + LANES), bf16),
            pltpu.VMEM((N_GROUPS, rows, width), f32),
            pltpu.VMEM((N_GROUPS, rows, width), bf16),
            pltpu.VMEM((N_GROUPS, rows, width), bf16),
            pltpu.VMEM((N_GROUPS, rows, width), bf16),
            pltpu.VMEM((N_GROUPS, rows, width), bf16),
            pltpu.VMEM((2, width, half), bf16),
            pltpu.VMEM((2, width, half), bf16),
            pltpu.VMEM((2, half, width), bf16),
            pltpu.VMEM((n_tok, N_GROUPS * rows), bf16),
            dma((4,)), dma((3,)), dma((3,)),
        ] + [dma((N_GROUPS, 4))] * 8,
        compiler_params=pltpu.CompilerParams(
            collective_id=0, has_side_effects=True, vmem_limit_bytes=67043328
        ),
        name="expert_layer",
    )(tokens, norm_gain.reshape(1, width), expert_ids.T, gate_weights.T, w_gate, w_up, w_down)


def solution(mesh):
    placed = (
        P(("grp", "ep", "tp"), None),
        P(),
        P(("grp", "ep", "tp"), None),
        P(("grp", "ep", "tp"), None),
        P("ep", None, "tp"),
        P("ep", None, "tp"),
        P("ep", "tp", None),
    )
    return jax.shard_map(
        shards, mesh=mesh, in_specs=placed, out_specs=P(("grp", "ep", "tp"), None), check_vma=False
    )
```
